32 devices in a mesh: rep: 2 (over x), fs: 4 (over z), tp: 4 (over y, core).
Axes of the slice: x: 2, y: 2, z: 4, core: 2. Of those that a mesh axis runs over, the one named last changes fastest.
Arguments:
- tokens: bfloat16 [8192, 2048], P(('rep', 'fs'), 'tp'), may hold values from -6 to 6
- mix_in_gain: bfloat16 [2048], replicated, may hold values from 0.099609375 to 1.8984375
- bgate_weight: bfloat16 [2048, 2048], P('fs', 'tp'), may hold values from -0.125 to 0.125
- cgate_weight: bfloat16 [2048, 2048], P('fs', 'tp'), may hold values from -0.125 to 0.125
- value_weight: bfloat16 [2048, 2048], P('fs', 'tp'), may hold values from -0.125 to 0.125
- conv_taps: bfloat16 [3, 2048], replicated, may hold values from -3 to 3
- out_weight: bfloat16 [2048, 2048], P('tp', 'fs'), may hold values from -0.41984465 to 0.41984465
- mix_out_gain: bfloat16 [2048], replicated, may hold values from 0.099609375 to 1.8984375
- ffn_in_gain: bfloat16 [2048], replicated, may hold values from 0.099609375 to 1.8984375
- up_weight: bfloat16 [2048, 8192], P('fs', 'tp'), may hold values from -0.125 to 0.125
- down_weight: bfloat16 [8192, 2048], P('tp', 'fs'), may hold values from -0.20992233 to 0.20992233
- ffn_out_gain: bfloat16 [2048], replicated, may hold values from 0.099609375 to 1.8984375
Outputs:
- result: bfloat16 [8192, 2048], P(('rep', 'fs'), 'tp')
The draws below stay inside these ranges and needn't reach their ends.
All inputs are finite; a program needn't handle non-finite values.
Results may differ from the reference program's by a relative error of at most 0.02.
Values may be sent and summed in bfloat16 or wider, within the bound.
No kernel may reach another device: no remote copies, remote signals or barrier semaphores. Data moves between devices by JAX's collectives and lax.ppermute only.
A program may use at most 128 MiB of HBM per device.

```python
import jax
import jax.numpy as jnp
from jax import lax

D = 2048
CW = 2048
FF = 8192
LEN = 256
TOKENS = 8192
N_TP = 4


def rising_matrix(base, rows, cols, top):
    ramp = top ** (jnp.arange(cols, dtype=jnp.float32) / cols)
    return (base * ramp[None, :] * rows ** (-0.5)).astype(jnp.bfloat16)


def draw_out_weight(key, part):
    own_key = jax.random.fold_in(key, 11)
    base = jnp.clip(jax.random.normal(own_key, (CW, D), jnp.float32), -6.0, 6.0)
    return rising_matrix(base, CW, D, 3.0)


def draw_down_weight(key, part):
    own_key = jax.random.fold_in(key, 23)
    base = jnp.clip(jax.random.normal(own_key, (FF, D), jnp.float32), -6.0, 6.0)
    return rising_matrix(base, FF, D, 3.0)


def shard_levels(key, extent, split, least, top_value):
    def one(position, blocks):
        steps = jax.random.uniform(jax.random.fold_in(jax.random.fold_in(key, 6), position), (blocks,), jnp.float32, least / len(split), top_value / len(split))
        return jnp.repeat(jnp.exp(steps), extent[position] // blocks).reshape((-1,) + (1,) * (len(extent) - position - 1))

    level = one(*split[0])
    for cut in split[1:]:
        level = level * one(*cut)
    return level


def centred(key, extent, spread, reach, split=(), kind=jnp.bfloat16):
    level = shard_levels(key, extent, split, -0.22, 0.18) if split else 1.0
    drawn = jax.random.normal(key, extent, jnp.float32) * spread * level
    return jnp.minimum(jnp.maximum(drawn, -reach), reach).astype(kind)


def setup_inputs(seed: int = 0) -> dict:
    arg_keys = jax.random.split(jax.random.key(seed), 13)
    return {
        "tokens": centred(arg_keys[0], (TOKENS, D), 1.0, 6.0, ((0, 8), (1, 4))),
        "mix_in_gain": jnp.clip(1.0 + 0.18 * jax.random.normal(arg_keys[1], (D,), jnp.float32), 0.099609375, 1.8984375).astype(jnp.bfloat16),
        "bgate_weight": centred(arg_keys[2], (D, CW), D ** -0.5, 0.125, ((0, 4), (1, 4))),
        "cgate_weight": centred(arg_keys[3], (D, CW), D ** -0.5, 0.125, ((0, 4), (1, 4))),
        "value_weight": centred(arg_keys[4], (D, CW), D ** -0.5, 0.125, ((0, 4), (1, 4))),
        "conv_taps": centred(arg_keys[5], (3, CW), 0.6, 3.0),
        "out_weight": draw_out_weight(jax.random.fold_in(arg_keys[12], 71), 0),
        "mix_out_gain": jnp.clip(1.0 + 0.18 * jax.random.normal(arg_keys[7], (D,), jnp.float32), 0.099609375, 1.8984375).astype(jnp.bfloat16),
        "ffn_in_gain": jnp.clip(1.0 + 0.18 * jax.random.normal(arg_keys[8], (D,), jnp.float32), 0.099609375, 1.8984375).astype(jnp.bfloat16),
        "up_weight": centred(arg_keys[9], (D, FF), D ** -0.5, 0.125, ((0, 4), (1, 4))),
        "down_weight": draw_down_weight(jax.random.fold_in(arg_keys[12], 71), 0),
        "ffn_out_gain": jnp.clip(1.0 + 0.18 * jax.random.normal(arg_keys[11], (D,), jnp.float32), 0.099609375, 1.8984375).astype(jnp.bfloat16),
    }


epsilon = 1e-06

def normalize(rows, gain):
    rows = rows.astype(jnp.float32)
    factor = lax.rsqrt(lax.optimization_barrier(jnp.mean(rows * rows, axis=-1, keepdims=True)) + epsilon)
    return rows * factor * gain.astype(jnp.float32)

def block_sum(left, right, blocks):
    width = left.shape[1] // blocks

    def step(total, index):
        start = (index * width).astype(jnp.int32)
        piece_left = lax.dynamic_slice_in_dim(left, start, width, 1)
        piece_right = lax.dynamic_slice_in_dim(right, start, width, 0)
        partial_term = jnp.dot(piece_left, piece_right, preferred_element_type=jnp.float32).astype(jnp.bfloat16)
        return (total + partial_term.astype(jnp.float32), None)
    start_total = jnp.zeros((left.shape[0], right.shape[1]), jnp.float32)
    total, _ = lax.scan(step, start_total, jnp.arange(blocks, dtype=jnp.int32))
    return total

def convolve(inner, taps):
    seqs = inner.reshape(-1, LEN, inner.shape[1])
    padded = jnp.pad(seqs, ((0, 0), (1, 1), (0, 0)))
    weights = taps.astype(jnp.float32)
    out = weights[0] * padded[:, :-2] + weights[1] * padded[:, 1:-1] + weights[2] * padded[:, 2:]
    return out.reshape(inner.shape)

def reference(tokens, mix_in_gain, bgate_weight, cgate_weight, value_weight, conv_taps, out_weight, mix_out_gain, ffn_in_gain, up_weight, down_weight, ffn_out_gain):
    normed = normalize(tokens, mix_in_gain).astype(jnp.bfloat16)
    bgate = jnp.dot(normed, bgate_weight, preferred_element_type=jnp.float32).astype(jnp.bfloat16)
    cgate = jnp.dot(normed, cgate_weight, preferred_element_type=jnp.float32).astype(jnp.bfloat16)
    value = jnp.dot(normed, value_weight, preferred_element_type=jnp.float32).astype(jnp.bfloat16)
    inner = cgate.astype(jnp.float32) * value.astype(jnp.float32)
    gated = (bgate.astype(jnp.float32) * convolve(inner, conv_taps)).astype(jnp.bfloat16)
    mixed = block_sum(gated, out_weight, N_TP)
    resid = (tokens.astype(jnp.float32) + normalize(mixed, mix_out_gain)).astype(jnp.bfloat16)
    second = normalize(resid, ffn_in_gain).astype(jnp.bfloat16)
    lifted = jnp.dot(second, up_weight, preferred_element_type=jnp.float32)
    active = jnp.square(jnp.maximum(lifted, 0.0)).astype(jnp.bfloat16)
    ffn = block_sum(active, down_weight, N_TP)
    return (resid.astype(jnp.float32) + normalize(ffn, ffn_out_gain)).astype(jnp.bfloat16)
```

```python
import jax
import jax.numpy as jnp
from jax import lax
from jax.sharding import PartitionSpec as P

LEN = 256
LANES = 128
UP_PIECES = 2


epsilon = 1e-06


def rms(rows, gain):
    rows = rows.astype(jnp.float32)
    factor = lax.rsqrt(jnp.mean(rows * rows, axis=-1, keepdims=True) + epsilon)
    return rows * factor * gain.astype(jnp.float32)


def convolve(inner, taps):
    seqs = inner.reshape(-1, LEN, inner.shape[1])
    padded = jnp.pad(seqs, ((0, 0), (1, 1), (0, 0)))
    weights = taps.astype(jnp.float32)
    out = weights[0] * padded[:, :-2] + weights[1] * padded[:, 1:-1] + weights[2] * padded[:, 2:]
    return out.reshape(inner.shape)


def add(left, right):
    return left.astype(jnp.float32) + right.astype(jnp.float32)


def make_body(n_rep, n_fs, n_tp):
    assert n_rep == 2 and n_tp & (n_tp - 1) == 0
    swap_pairs = [(0, 1), (1, 0)]
    bits = [1 << k for k in range(n_tp.bit_length() - 1)]

    def flip(value, bit):
        return lax.ppermute(value, "tp", [(i, i ^ bit) for i in range(n_tp)])

    def ordered(mine, other, on, axis):
        first = jnp.where(on == 0, mine, other)
        second = jnp.where(on == 0, other, mine)
        return jnp.stack([first, second], axis=axis)

    def spread(block, column):
        value = block[:, None, :]
        for bit in reversed(bits):
            on = (column // bit) % 2
            other = flip(value, bit)
            value = ordered(value, other, on, 2).reshape(block.shape[0], -1, block.shape[1])
        return value.reshape(block.shape[0], -1)

    def half_sum(blocks, column):
        rows, _, width = blocks.shape
        parts = blocks.reshape(rows, n_tp // 2, 2, width)
        on = column % 2
        keep = lax.dynamic_index_in_dim(parts, on, 2, keepdims=False)
        send = lax.dynamic_index_in_dim(parts, 1 - on, 2, keepdims=False)
        return add(keep, flip(send, 1))

    def sum_all(partial, column):
        rows, full = partial.shape
        total = half_sum(partial.reshape(rows, n_tp, full // n_tp), column)
        for bit in bits[1:]:
            total = total.astype(jnp.bfloat16)
            total = add(total, flip(total, bit))
        total = total.astype(jnp.bfloat16)
        other = flip(total, 1)
        return ordered(total, other, column % 2, 2).reshape(rows, full)

    def sum_scatter(blocks, column):
        total = half_sum(blocks, column)
        for bit in reversed(bits[1:]):
            total = total.astype(jnp.bfloat16)
            rows, count, width = total.shape
            parts = total.reshape(rows, 2, count // 2, width)
            on = (column // bit) % 2
            keep = lax.dynamic_index_in_dim(parts, on, 1, keepdims=False)
            send = lax.dynamic_index_in_dim(parts, 1 - on, 1, keepdims=False)
            total = add(keep, flip(send, bit))
        return total[:, 0]

    def body(
        tokens,
        mix_in_gain,
        bgate_weight,
        cgate_weight,
        value_weight,
        conv_taps,
        out_weight,
        mix_out_gain,
        ffn_in_gain,
        up_weight,
        down_weight,
        ffn_out_gain,
    ):
        column = lax.axis_index("tp")
        group = lax.axis_index("rep")
        own_width = tokens.shape[1]
        first = column * own_width
        full_width = mix_in_gain.shape[0]

        def half(array, axis, which):
            size = array.shape[axis] // 2
            return lax.dynamic_slice_in_dim(array, which * size, size, axis)

        def both(piece, axis):
            near = lax.all_gather(piece, "fs", axis=axis, tiled=True)
            far = lax.ppermute(near, "rep", swap_pairs)
            return near, far

        gates = jnp.concatenate(
            [half(w, 1, group) for w in (bgate_weight, cgate_weight, value_weight)], axis=1
        )
        gates = both(gates, 0)
        outs = both(half(out_weight, 0, group), 1)
        up_half = half(up_weight, 1, group)
        step = up_half.shape[1] // UP_PIECES
        ups = [both(up_half[:, k * step : (k + 1) * step], 0) for k in range(UP_PIECES)]
        down_half = half(down_weight, 0, group)
        shard = down_half.shape[1]
        pieces = shard // LANES if n_fs % n_tp == 0 and shard % LANES == 0 else 1
        wide = shard // pieces
        downs = [both(down_half[:, k * wide : (k + 1) * wide], 1) for k in range(pieces)]

        whole = spread(tokens, column)
        normed = rms(whole, mix_in_gain).astype(jnp.bfloat16)
        channels = bgate_weight.shape[1]
        own_taps = lax.dynamic_slice_in_dim(conv_taps, column * channels, channels, 1)
        partial_mix = 0.0
        for which, weight, out in zip((group, 1 - group), gates, outs):
            projected = jnp.dot(normed, weight, preferred_element_type=jnp.float32)
            bgate, cgate, value = jnp.split(projected.astype(jnp.bfloat16), 3, axis=1)
            inner = cgate.astype(jnp.float32) * value.astype(jnp.float32)
            mixed_in = convolve(inner, half(own_taps, 1, which))
            gated = (bgate.astype(jnp.float32) * mixed_in).astype(jnp.bfloat16)
            partial_mix = partial_mix + jnp.dot(gated, out, preferred_element_type=jnp.float32)
        mixed = sum_all(partial_mix.astype(jnp.bfloat16), column)
        resid = add(whole, rms(mixed, mix_out_gain)).astype(jnp.bfloat16)
        resid_own = lax.dynamic_slice_in_dim(resid, first, own_width, 1)
        second = rms(resid, ffn_in_gain).astype(jnp.bfloat16)

        def activate(weight):
            lifted = jnp.dot(second, weight, preferred_element_type=jnp.float32)
            return jnp.square(jnp.maximum(lifted, 0.0)).astype(jnp.bfloat16)

        active = [
            jnp.concatenate([activate(pair[side]) for pair in ups], axis=1) for side in range(2)
        ]
        own = []
        for near, far in downs:
            partial = jnp.dot(active[0], near, preferred_element_type=jnp.float32)
            partial = partial + jnp.dot(active[1], far, preferred_element_type=jnp.float32)
            partial = partial.astype(jnp.bfloat16).reshape(partial.shape[0], n_tp, -1)
            own.append(sum_scatter(partial, column).reshape(partial.shape[0], -1, wide))
        ffn = jnp.stack(own, axis=2).reshape(-1, own_width) if pieces > 1 else own[0].reshape(-1, own_width)
        ffn_energy = lax.psum(jnp.sum(ffn * ffn, axis=1), "tp")
        out_gain = lax.dynamic_slice_in_dim(ffn_out_gain, first, own_width, 0).astype(jnp.float32)
        closing = ffn * lax.rsqrt(ffn_energy[:, None] / full_width + epsilon) * out_gain
        return add(resid_own, closing).astype(jnp.bfloat16)

    return body


def solution(mesh):
    placed = (
        P(("rep", "fs"), "tp"),
        P(),
        P("fs", "tp"),
        P("fs", "tp"),
        P("fs", "tp"),
        P(),
        P("tp", "fs"),
        P(),
        P(),
        P("fs", "tp"),
        P("tp", "fs"),
        P(),
    )
    body = make_body(mesh.shape["rep"], mesh.shape["fs"], mesh.shape["tp"])
    return jax.shard_map(
        body, mesh=mesh, in_specs=placed, out_specs=P(("rep", "fs"), "tp"), check_vma=False
    )
```

```python
import jax
import jax.numpy as jnp
from jax import lax
from jax.sharding import PartitionSpec as P


LEN = 256
LANES = 128
UP_PIECES = 2
DOWN_PIECES = 2


epsilon = 1e-06


def rms(rows, gain):
    rows = rows.astype(jnp.float32)
    factor = lax.rsqrt(jnp.mean(rows * rows, axis=-1, keepdims=True) + epsilon)
    return rows * factor * gain.astype(jnp.float32)


def convolve(inner, taps):
    seqs = inner.reshape(-1, LEN, inner.shape[1])
    padded = jnp.pad(seqs, ((0, 0), (1, 1), (0, 0)))
    weights = taps.astype(jnp.float32)
    out = weights[0] * padded[:, :-2] + weights[1] * padded[:, 1:-1] + weights[2] * padded[:, 2:]
    return out.reshape(inner.shape)


def add(left, right):
    return left.astype(jnp.float32) + right.astype(jnp.float32)


def make_body(n_rep, n_fs, n_tp):
    assert n_rep == 2 and n_tp & (n_tp - 1) == 0
    swap_pairs = [(0, 1), (1, 0)]
    bits = [1 << k for k in range(n_tp.bit_length() - 1)]

    def flip(value, bit):
        return lax.ppermute(value, "tp", [(i, i ^ bit) for i in range(n_tp)])

    def on(column, bit):
        return (column & bit) == 0

    def split(value, count):
        width = value.shape[1] // count
        return [value[:, k * width : (k + 1) * width] for k in range(count)]

    def join(blocks):
        return jnp.concatenate(blocks, axis=1) if len(blocks) > 1 else blocks[0]

    def merge(mine, other, zero, count):
        pairs = zip(split(mine, count), split(other, count))
        return join(
            [part for m, o in pairs for part in (jnp.where(zero, m, o), jnp.where(zero, o, m))]
        )

    def choose(blocks, zero):
        pairs = [(blocks[k], blocks[k + 1]) for k in range(0, len(blocks), 2)]
        keep = join([jnp.where(zero, first, second) for first, second in pairs])
        send = join([jnp.where(zero, second, first) for first, second in pairs])
        return keep, send

    def spread(block, column):
        value, count = block, 1
        for bit in reversed(bits):
            value = merge(value, flip(value, bit), on(column, bit), count)
            count *= 2
        return value

    def half_sum(partial, column):
        keep, send = choose(split(partial, n_tp), on(column, 1))
        return add(keep, flip(send, 1))

    def sum_all(partial, column):
        total = half_sum(partial, column).astype(jnp.bfloat16)
        for bit in bits[1:]:
            other = flip(total, bit)
            total = add(total, other).astype(jnp.bfloat16)
        return merge(total, flip(total, 1), on(column, 1), n_tp // 2)

    def sum_scatter(partial, column):
        total, count = half_sum(partial, column), n_tp // 2
        for bit in bits[1:]:
            keep, send = choose(split(total.astype(jnp.bfloat16), count), on(column, bit))
            total, count = add(keep, flip(send, bit)), count // 2
        return total

    def body(
        tokens,
        mix_in_gain,
        bgate_weight,
        cgate_weight,
        value_weight,
        conv_taps,
        out_weight,
        mix_out_gain,
        ffn_in_gain,
        up_weight,
        down_weight,
        ffn_out_gain,
    ):
        column = lax.axis_index("tp")
        group = lax.axis_index("rep")
        own_width = tokens.shape[1]
        first = column * own_width
        full_width = mix_in_gain.shape[0]

        def half(array, axis, which):
            size = array.shape[axis] // 2
            return lax.dynamic_slice_in_dim(array, which * size, size, axis)

        def both(piece, axis):
            near = lax.all_gather(piece, "fs", axis=axis, tiled=True)
            far = lax.ppermute(near, "rep", swap_pairs)
            return near, far

        gates = jnp.concatenate(
            [half(w, 1, group) for w in (bgate_weight, cgate_weight, value_weight)], axis=1
        )
        gates = both(gates, 0)
        outs = both(half(out_weight, 0, group), 1)
        up_half = half(up_weight, 1, group)
        step = up_half.shape[1] // UP_PIECES
        ups = [both(up_half[:, k * step : (k + 1) * step], 0) for k in range(UP_PIECES)]
        down_half = half(down_weight, 0, group)
        shard = down_half.shape[1]
        pieces = DOWN_PIECES if n_fs % n_tp == 0 and shard % (DOWN_PIECES * LANES) == 0 else 1
        wide = shard // pieces
        downs = []
        for k in range(pieces):
            near = down_half[:, k * wide : (k + 1) * wide]
            if k and k == pieces - 1:
                rest = half(down_weight, 0, 1 - group)[:, k * wide : (k + 1) * wide]
                near = lax.all_gather(near, "fs", axis=1, tiled=True)
                far = lax.all_gather(rest, "fs", axis=1, tiled=True)
                downs.append((near, far))
            else:
                downs.append(both(near, 1))

        whole = spread(tokens, column)
        normed = rms(whole, mix_in_gain).astype(jnp.bfloat16)
        channels = bgate_weight.shape[1]
        own_taps = lax.dynamic_slice_in_dim(conv_taps, column * channels, channels, 1)
        partial_mix = 0.0
        for which, weight, out in zip((group, 1 - group), gates, outs):
            projected = jnp.dot(normed, weight, preferred_element_type=jnp.float32)
            bgate, cgate, value = jnp.split(projected.astype(jnp.bfloat16), 3, axis=1)
            inner = cgate.astype(jnp.float32) * value.astype(jnp.float32)
            mixed_in = convolve(inner, half(own_taps, 1, which))
            gated = (bgate.astype(jnp.float32) * mixed_in).astype(jnp.bfloat16)
            partial_mix = partial_mix + jnp.dot(gated, out, preferred_element_type=jnp.float32)
        mixed = sum_all(partial_mix.astype(jnp.bfloat16), column)
        resid = add(whole, rms(mixed, mix_out_gain)).astype(jnp.bfloat16)
        resid_own = lax.dynamic_slice_in_dim(resid, first, own_width, 1)
        second = rms(resid, ffn_in_gain).astype(jnp.bfloat16)

        def activate(weight):
            lifted = jnp.dot(second, weight, preferred_element_type=jnp.float32)
            return jnp.square(jnp.maximum(lifted, 0.0)).astype(jnp.bfloat16)

        active = [
            jnp.concatenate([activate(pair[side]) for pair in ups], axis=1) for side in range(2)
        ]
        own = []
        for near, far in downs:
            partial = jnp.dot(active[0], near, preferred_element_type=jnp.float32)
            partial = partial + jnp.dot(active[1], far, preferred_element_type=jnp.float32)
            own.append(sum_scatter(partial.astype(jnp.bfloat16), column))
        runs = [split(piece, own_width // shard if pieces > 1 else 1) for piece in own]
        ffn = join([run for turn in zip(*runs) for run in turn])
        ffn_energy = lax.psum(jnp.sum(ffn * ffn, axis=1), "tp")
        out_gain = lax.dynamic_slice_in_dim(ffn_out_gain, first, own_width, 0).astype(jnp.float32)
        closing = ffn * lax.rsqrt(ffn_energy[:, None] / full_width + epsilon) * out_gain
        return add(resid_own, closing).astype(jnp.bfloat16)

    return body


def solution(mesh):
    placed = (
        P(("rep", "fs"), "tp"),
        P(),
        P("fs", "tp"),
        P("fs", "tp"),
        P("fs", "tp"),
        P(),
        P("tp", "fs"),
        P(),
        P(),
        P("fs", "tp"),
        P("tp", "fs"),
        P(),
    )
    body = make_body(mesh.shape["rep"], mesh.shape["fs"], mesh.shape["tp"])
    return jax.shard_map(
        body, mesh=mesh, in_specs=placed, out_specs=P(("rep", "fs"), "tp"), check_vma=False
    )
```
